256 devices in a mesh: ep: 64 (over z, y, core), tp: 4 (over x).
Axes of the slice: x: 4, y: 4, z: 8, core: 2. Of those that a mesh axis runs over, the one named last changes fastest.
Arguments:
- tokens: bfloat16 [2048, 2048], P('ep'), may hold values from -6 to 6
- gain_mix: bfloat16 [2048], replicated, may hold values from 0.099609375 to 1.8984375
- gain_ffn: bfloat16 [2048], replicated, may hold values from 0.099609375 to 1.8984375
- w_query: bfloat16 [2048, 1024], P('ep', 'tp'), may hold values from -0.125 to 0.125
- w_key: bfloat16 [2048, 1024], P('ep', 'tp'), may hold values from -0.125 to 0.125
- w_value: bfloat16 [2048, 1024], P('ep', 'tp'), may hold values from -0.125 to 0.125
- w_outgate: bfloat16 [2048, 1024], P('ep', 'tp'), may hold values from -0.125 to 0.125
- w_ingate: bfloat16 [2048, 8], replicated, may hold values from -0.125 to 0.125
- w_forget: bfloat16 [2048, 8], replicated, may hold values from -0.125 to 0.125
- bias_in: float32 [8], replicated, may hold values from -2 to 2
- bias_forget: float32 [8], replicated, may hold values from -1 to 3
- w_proj: bfloat16 [1024, 2048], P('tp'), may hold values from -0.1875 to 0.1875
- matrix_state: float32 [2048, 8, 128, 128], P('ep', 'tp'), may hold values from -0.6 to 0.6
- normal_state: float32 [2048, 8, 128], P('ep', 'tp'), may hold values from -0.6 to 0.6
- stab_state: float32 [2048, 8], P('ep', 'tp'), may hold values from -1 to 1
- route_ids: int32 [2048, 2], P('ep'), may hold values from 0 to 31, all different within a row; in each aligned block of 32 rows (0 to 31, 32 to 63, ...) at most 4 rows name the same one
- route_weights: float32 [2048, 2], P('ep'), may hold values from 0.1 to 1
- w_exp_gate: bfloat16 [64, 2048, 1536], P('ep', None, 'tp'), may hold values from -0.125 to 0.125
- w_exp_up: bfloat16 [64, 2048, 1536], P('ep', None, 'tp'), may hold values from -0.125 to 0.125
- w_exp_down: bfloat16 [64, 1536, 2048], P('ep', 'tp'), may hold values from -0.109375 to 0.109375
Outputs:
- mixed_out: bfloat16 [2048, 2048], P('ep', 'tp')
- matrix_out: float32 [2048, 8, 128, 128], P('ep', 'tp')
- normal_out: float32 [2048, 8, 128], P('ep', 'tp')
- stab_out: float32 [2048, 8], P('ep', 'tp')
The draws below stay inside these ranges and needn't reach their ends.
Inputs may be any that keep to these rules, and one draw needn't show every extreme that they name: `route_ids`: each row names 2 different experts; among the rows of one index of ep no expert is named by more than 4 rows, and in every draw some expert is named by exactly 4 of them.
All inputs are finite; a program needn't handle non-finite values.
Results may differ from the reference program's by a relative error of at most 0.015.
Values may be sent and summed in bfloat16 or wider, within the bound.
A program may use at most 64 MiB of HBM per device.

```python
import math
import jax
import jax.numpy as jnp
import numpy as np
from jax import lax

D = 2048
HEADS = 8
HEAD_DIM = 128
FF = 3072
TOPK = 2
SEQ_DEV = 32
WIDTH = 1024
SEQS = 2048
EXPERTS = 32
CAP = 4
N_EP = 64
N_TP = 4


def shard_levels(stream_key, extent, split, low, largest):
    level = 1.0
    for dim, shards_of in split:
        draws = jax.random.uniform(jax.random.fold_in(jax.random.fold_in(stream_key, 6), dim), (shards_of,), jnp.float32, low / len(split), largest / len(split))
        level = level * jnp.repeat(jnp.exp(draws), extent[dim] // shards_of).reshape((-1,) + (1,) * (len(extent) - 1 - dim))
    return level


def shared_out(own_key, own, number, rows, count, top, most, lean):
    order = jax.random.permutation(own_key, count)
    heavy_load, common = portions_of(count, rows * top, most, lean, True), portions_of(count, rows * top, most, lean, False)
    places = jnp.arange(count)

    def named(tallies, turn):
        used = int((tallies > 0).sum())
        fixed = max(1, used // 4)
        moved = fixed + (places - fixed + turn * (used - fixed)) % max(1, count - fixed)
        return jnp.zeros((count,), jnp.int32).at[order[jnp.where(places < fixed, places, moved)]].set(jnp.asarray(tallies, jnp.int32))

    tallies = jnp.where(number % 4 == 0, named(heavy_load, number // 4), named(common, number - number // 4 - 1))
    mixed = jax.random.permutation(jax.random.fold_in(own, 3), count)
    donor, sink = mixed[0:count // 2 * 2:2], mixed[1:count // 2 * 2:2]
    room = jnp.minimum(tallies[donor] - 1, most - tallies[sink]) // 2
    room = jnp.where((donor == order[0]) | (sink == order[0]) | (tallies[sink] == 0), 0, jnp.maximum(room, 0))
    moved = jax.random.randint(jax.random.fold_in(own, 4), (count // 2,), 0, 1 << 20) % (room + 1)
    tallies = tallies.at[donor].add(-moved).at[sink].add(moved)
    items = jnp.searchsorted(jnp.cumsum(tallies), jnp.arange(rows * top), side="right").astype(jnp.int32)
    table = items.reshape(top, rows).T
    table = table[jax.random.permutation(jax.random.fold_in(own, 1), rows)]
    turn = jax.random.randint(jax.random.fold_in(own, 2), (rows, 1), 0, top)
    return jnp.take_along_axis(table, (jnp.arange(top)[None, :] + turn) % top, axis=1)


def portions_of(number_of, total, most, lean, full):
    portions = [(1 << 20) // math.isqrt(grade ** lean) + 1 for grade in range(1, number_of + 1)]
    largest = most if full else min(most, max(-(-total // number_of), total * portions[0] // sum(portions)))
    least = 1 if total - largest >= number_of - 1 else 0
    holding, surplus = [largest] + [least] * (number_of - 1), total - largest - least * (number_of - 1)
    while surplus > 0:
        movable = [i for i in range(1, number_of) if holding[i] < largest] or [i for i in range(1, number_of) if holding[i] < most]
        mass, budget = sum([portions[i] for i in movable]), surplus
        for i in movable:
            extra = min(most - holding[i], max(1, budget * portions[i] // mass), surplus)
            holding[i] = holding[i] + extra
            surplus = surplus - extra
    return np.array(holding)


def scatter_about(stream_key, dims, width, reach, split=(), held_as=jnp.bfloat16):
    level = shard_levels(stream_key, dims, split, -0.22, 0.18) if split else 1.0
    values = jax.random.normal(stream_key, dims, jnp.float32) * width * level
    return jnp.minimum(jnp.maximum(values, -reach), reach).astype(held_as)


def setup_inputs(seed: int = 0) -> dict:
    splits = jax.random.split(jax.random.key(seed), 21)
    tokens = scatter_about(splits[0], (SEQS, D), 1.0, 6.0, ((0, 64),))
    gain_mix = jnp.clip(1.0 + 0.18 * jax.random.normal(splits[1], (D,), jnp.float32), 0.099609375, 1.8984375).astype(jnp.bfloat16)
    gain_ffn = jnp.clip(1.0 + 0.18 * jax.random.normal(splits[2], (D,), jnp.float32), 0.099609375, 1.8984375).astype(jnp.bfloat16)
    w_query = scatter_about(splits[3], (D, WIDTH), D ** -0.5, 0.125, ((0, 64), (1, 4)))
    w_key = scatter_about(splits[4], (D, WIDTH), D ** -0.5, 0.125, ((0, 64), (1, 4)))
    w_value = scatter_about(splits[5], (D, WIDTH), D ** -0.5, 0.125, ((0, 64), (1, 4)))
    w_outgate = scatter_about(splits[6], (D, WIDTH), D ** -0.5, 0.125, ((0, 64), (1, 4)))
    w_ingate = scatter_about(splits[7], (D, HEADS), D ** -0.5, 0.125)
    w_forget = scatter_about(splits[8], (D, HEADS), D ** -0.5, 0.125)
    bias_in = jnp.clip(jax.random.uniform(splits[9], (HEADS,), jnp.float32, -2.0, 2.0), -2.0, 2.0)
    bias_forget = jnp.clip(jax.random.uniform(splits[10], (HEADS,), jnp.float32, -1.0, 3.0), -1.0, 3.0)
    w_proj = scatter_about(splits[11], (WIDTH, D), WIDTH ** -0.5, 0.1875, ((0, 4),))
    matrix_state = scatter_about(splits[12], (SEQS, HEADS, HEAD_DIM, HEAD_DIM), 0.1, 0.6, ((0, 64), (1, 4)), jnp.float32)
    normal_state = scatter_about(splits[13], (SEQS, HEADS, HEAD_DIM), 0.1, 0.6, ((0, 64), (1, 4)), jnp.float32)
    stab_state = jnp.clip(jax.random.uniform(splits[14], (SEQS, HEADS), jnp.float32, -1.0, 1.0) * shard_levels(splits[14], (SEQS, HEADS), ((0, 64), (1, 4)), -0.4, 0.0), -1.0, 1.0)
    route_ids_keys = jax.random.split(jax.random.fold_in(splits[15], 1), SEQS // SEQ_DEV)
    route_ids_turns = jax.random.permutation(jax.random.fold_in(splits[15], 3), SEQS // SEQ_DEV)
    route_ids = jax.vmap(lambda own, number: shared_out(jax.random.fold_in(splits[15], 2), own, number, SEQ_DEV, EXPERTS, TOPK, CAP, 1))(route_ids_keys, route_ids_turns).reshape((SEQS, TOPK))
    route_weights = jnp.clip(0.1 + 0.9 * jax.random.uniform(splits[16], (SEQS, TOPK), jnp.float32) ** shard_levels(splits[16], (SEQS, TOPK), ((0, 64),), -0.2, 0.2), 0.1, 1.0)
    w_exp_gate = scatter_about(splits[17], (2 * EXPERTS, D, FF // 2), D ** -0.5, 0.125, ((0, 64), (2, 4)))
    w_exp_up = scatter_about(splits[18], (2 * EXPERTS, D, FF // 2), D ** -0.5, 0.125, ((0, 64), (2, 4)))
    w_exp_down = scatter_about(splits[19], (2 * EXPERTS, FF // 2, D), FF ** -0.5, 0.109375, ((0, 64), (1, 4)))
    return {"tokens": tokens, "gain_mix": gain_mix, "gain_ffn": gain_ffn, "w_query": w_query, "w_key": w_key, "w_value": w_value, "w_outgate": w_outgate, "w_ingate": w_ingate, "w_forget": w_forget, "bias_in": bias_in, "bias_forget": bias_forget, "w_proj": w_proj, "matrix_state": matrix_state, "normal_state": normal_state, "stab_state": stab_state, "route_ids": route_ids, "route_weights": route_weights, "w_exp_gate": w_exp_gate, "w_exp_up": w_exp_up, "w_exp_down": w_exp_down}


norm_epsilon = 1e-06

def rms_scale(row_block, gain):
    wide = row_block.astype(jnp.float32)
    factor = lax.rsqrt(lax.optimization_barrier(jnp.mean(wide * wide, axis=-1, keepdims=True)) + norm_epsilon)
    return (wide * factor * gain.astype(jnp.float32)).astype(jnp.bfloat16)

def memory_step(query, key_rows, value_rows, gate_rows, in_pre, forget_pre, matrix_state, normal_state, stab_state):
    log_forget = jax.nn.log_sigmoid(forget_pre)
    stab_new = jnp.maximum(log_forget + stab_state, in_pre)
    carry = jnp.exp(log_forget + stab_state - stab_new)
    inflow = jnp.exp(in_pre - stab_new)
    scaled_keys = key_rows.astype(jnp.float32) * query.shape[-1] ** (-0.5)
    value_wide = value_rows.astype(jnp.float32)
    matrix_new = carry[..., None, None] * matrix_state + inflow[..., None, None] * scaled_keys[..., :, None] * value_wide[..., None, :]
    normal_new = carry[..., None] * normal_state + inflow[..., None] * scaled_keys
    query_wide = query.astype(jnp.float32)
    numer = jnp.einsum('shd,shde->she', query_wide, matrix_new, precision=lax.Precision.HIGHEST)
    denom = jnp.maximum(jnp.abs(lax.optimization_barrier(jnp.sum(query_wide * normal_new, axis=-1))), 1.0)
    hidden = numer / denom[..., None] * jax.nn.sigmoid(gate_rows.astype(jnp.float32))
    return (hidden, matrix_new, normal_new, stab_new)

def reference(tokens, gain_mix, gain_ffn, w_query, w_key, w_value, w_outgate, w_ingate, w_forget, bias_in, bias_forget, w_proj, matrix_state, normal_state, stab_state, route_ids, route_weights, w_exp_gate, w_exp_up, w_exp_down):
    normed = rms_scale(tokens, gain_mix)

    def project(weight):
        return jnp.dot(normed, weight, preferred_element_type=jnp.float32).astype(jnp.bfloat16).reshape(SEQS, HEADS, HEAD_DIM)
    query = project(w_query)
    key_rows = project(w_key)
    value_rows = project(w_value)
    gate_rows = project(w_outgate)
    in_pre = jnp.dot(normed, w_ingate, preferred_element_type=jnp.float32) + bias_in
    forget_pre = jnp.dot(normed, w_forget, preferred_element_type=jnp.float32) + bias_forget
    hidden, matrix_new, normal_new, stab_new = memory_step(query, key_rows, value_rows, gate_rows, in_pre, forget_pre, matrix_state, normal_state, stab_state)
    cell = hidden.reshape(SEQS, WIDTH).astype(jnp.bfloat16)
    group_terms = jnp.einsum('sbw,bwd->bsd', cell.reshape(SEQS, N_TP, WIDTH // N_TP).astype(jnp.float32), w_proj.reshape(N_TP, WIDTH // N_TP, D).astype(jnp.float32))
    group_terms = lax.optimization_barrier(group_terms.astype(jnp.bfloat16))
    attended = lax.optimization_barrier(jnp.sum(group_terms.astype(jnp.float32), axis=0))
    resid = (tokens.astype(jnp.float32) + attended).astype(jnp.bfloat16)
    normed_ffn = rms_scale(resid, gain_ffn)
    flat_ids = route_ids.reshape(N_EP, SEQ_DEV * TOPK).astype(jnp.int32)
    expert_hot = (flat_ids[..., None] == jnp.arange(EXPERTS, dtype=jnp.int32)).astype(jnp.int32)
    slot_rank = lax.optimization_barrier(jnp.sum((jnp.cumsum(expert_hot, axis=1).astype(jnp.int32) - 1) * expert_hot, axis=-1)).astype(jnp.int32)
    placed = (jnp.arange(N_EP, dtype=jnp.int32)[:, None] * CAP + slot_rank).astype(jnp.int32)
    routed_rows = jnp.repeat(normed_ffn, TOPK, axis=0).reshape(N_EP, SEQ_DEV * TOPK, D)
    buffer = jnp.zeros((EXPERTS, N_EP * CAP, D), jnp.bfloat16).at[flat_ids, placed].set(routed_rows)
    quarter = FF // (2 * N_TP)

    def expert(operands):
        inputs, gate_pair, up_pair, down_pair = operands
        results = []
        for half_index in range(2):
            gate_sum = jnp.dot(inputs, gate_pair[half_index], preferred_element_type=jnp.float32)
            up_sum = jnp.dot(inputs, up_pair[half_index], preferred_element_type=jnp.float32)
            inner = (jax.nn.silu(gate_sum) * up_sum).astype(jnp.bfloat16)
            quarters = jnp.einsum('rtf,tfd->trd', inner.reshape(N_EP * CAP, N_TP, quarter).astype(jnp.float32), down_pair[half_index].reshape(N_TP, quarter, D).astype(jnp.float32))
            quarters = lax.optimization_barrier(quarters.astype(jnp.bfloat16))
            results.append(lax.optimization_barrier(jnp.sum(quarters.astype(jnp.float32), axis=0)).astype(jnp.bfloat16))
        return jnp.stack(results)
    outputs = lax.map(expert, (buffer, w_exp_gate.reshape(EXPERTS, 2, D, FF // 2), w_exp_up.reshape(EXPERTS, 2, D, FF // 2), w_exp_down.reshape(EXPERTS, 2, FF // 2, D)))
    picked = outputs[flat_ids, :, placed]
    both_halves = lax.optimization_barrier(jnp.sum(picked.astype(jnp.float32), axis=2)).reshape(SEQS, TOPK, D)
    weights = route_weights / lax.optimization_barrier(jnp.sum(route_weights, axis=-1, keepdims=True))
    routed = lax.optimization_barrier(jnp.sum(weights[..., None] * both_halves, axis=1))
    mixed_out = (resid.astype(jnp.float32) + routed).astype(jnp.bfloat16)
    return (mixed_out, matrix_new, normal_new, stab_new)
```

```python
import functools
import jax
import jax.numpy as jnp
from jax import lax
from jax.experimental import pallas as pl
from jax.experimental.pallas import tpu as pltpu
from jax.sharding import PartitionSpec as P

norm_epsilon = 1e-06
CAP = 4
LANES = 128
F32, BF16 = jnp.float32, jnp.bfloat16
MESH = pl.DeviceIdType.MESH


def iota(shape, dim):
    return lax.broadcasted_iota(jnp.int32, shape, dim)


def dot(a, b):
    return jnp.dot(a, b, preferred_element_type=F32)


def layer_kernel(
    cfg,
    tokens_h, gain_mix_h, gain_ffn_h, wq_h, wk_h, wv_h, wo_h, win_h, wfg_h, bias_in, bias_forget,
    wproj_h, mat_h, nrm_h, stab_h, ids_h, rw_h, wgate_h, wup_h, wdown_h,
    mixed_o, mat_o, nrm_o, stab_o,
    tok, gmix, gffn, win, wfg, wproj, mat, nrm, stab, ids, rw, wgu, wdown,
    wbuf, asend, arecv, psend, precv, normed, square, carry_b, vals_b, num, cell, gain32,
    asrc, adst, resid, table, table_hi, table_lo, dsrc, ddst, xrows0, xrows1, acc, csrc, cdst, own_sum,
    ssrc, sdst, rsrc, rdst,
    sems,
):
    nz, ny, nx, rows, depth, width, ffl, heads = cfg
    ep, t = lax.axis_index("ep"), lax.axis_index("tp")
    c = lax.rem(ep, 2)
    y = lax.rem(lax.div(ep, 2), ny)
    z = lax.div(ep, 2 * ny)
    chips = nz * ny
    quarter = width // nx
    blocks = quarter // LANES
    tile = blocks * CAP
    slots = chips * CAP
    head_dim = LANES
    cols = heads * head_dim

    def at(zz, yy):
        return (lax.rem(zz, nz) * ny + lax.rem(yy, ny)) * 2 + c

    def ahead(d):
        return at(z + lax.div(d, ny), y + lax.rem(d, ny))

    def behind(d):
        return at(z + nz - lax.div(d, ny), y + ny - lax.rem(d, ny))

    partner = ep + 1 - 2 * c
    used = [0]
    sending = []

    def sem():
        used[0] += 1
        return sems.at[used[0] - 1]

    def load(src, dst):
        copy = pltpu.make_async_copy(src, dst, sem())
        copy.start()
        return copy

    def remote(src, dst, to, recv=None):
        copy = pltpu.make_async_remote_copy(
            src_ref=src, dst_ref=dst, send_sem=sem(), recv_sem=sem() if recv is None else recv,
            device_id=to, device_id_type=MESH,
        )
        copy.start()
        sending.append(copy)
        return copy

    weights = [load(w, wbuf.at[z, c, :, i * cols:(i + 1) * cols]) for i, w in enumerate((wq_h, wk_h, wv_h, wo_h))]
    early = [load(a, b) for a, b in ((tokens_h, tok), (gain_mix_h, gmix), (ids_h, ids), (rw_h, rw), (win_h, win), (wfg_h, wfg), (stab_h, stab), (nrm_h, nrm), (gain_ffn_h, gffn))]
    mat_in = load(mat_h, mat)
    wproj_in = load(wproj_h, wproj)
    experts_in = [load(wgate_h.at[0], wgu.at[:, 0:ffl]), load(wup_h.at[0], wgu.at[:, ffl:2 * ffl]), load(wdown_h.at[0], wdown)]

    barrier = pltpu.get_barrier_semaphore()

    def greet(d, carry):
        pl.semaphore_signal(barrier, inc=1, device_id=(ahead(d), t), device_id_type=MESH)
        return carry

    lax.fori_loop(1, chips, greet, 0)
    for dx in range(1, nx):
        pl.semaphore_signal(barrier, inc=1, device_id=(ep, lax.rem(t + dx, nx)), device_id_type=MESH)
    pl.semaphore_signal(barrier, inc=1, device_id=(partner, t), device_id_type=MESH)
    pl.semaphore_wait(barrier, chips - 1 + nx - 1 + 1)

    for copy in weights:
        copy.wait()
    right, left = at(z + 1, y), at(z + nz - 1, y)
    pieces = 2
    pcols = 4 * cols // pieces
    reach = [(nz // 2, nz - 1 - nz // 2), (nz - 1 - nz // 2, nz // 2)]
    handed = sem()

    def piece(zz, p):
        return wbuf.at[lax.rem(zz, nz), c, :, p * pcols:(p + 1) * pcols]

    def hop(zz, p, to, recv):
        return remote(piece(zz, p), piece(zz, p), (to, t), recv)

    going_right, going_left = {}, {}
    recv_right = {(k, p): sem() for p in range(pieces) for k in range(1, reach[p][0] + 1)}
    recv_left = {(k, p): sem() for p in range(pieces) for k in range(1, reach[p][1] + 1)}
    for p in range(pieces):
        if reach[p][0] >= 1:
            going_right[(1, p)] = hop(z, p, right, recv_right[(1, p)])
        if reach[p][1] >= 1:
            going_left[(1, p)] = hop(z, p, left, recv_left[(1, p)])
    for p in range(pieces):
        hop(z, p, partner, handed)

    for copy in early:
        copy.wait()
    wide = tok[...].astype(F32)
    factor = lax.rsqrt(jnp.sum(wide * wide, axis=-1, keepdims=True) * (1.0 / width) + norm_epsilon)
    gain32[0] = gmix[...].astype(F32)
    gain32[1] = gffn[...].astype(F32)
    for b in range(width // LANES):
        here = slice(b * LANES, (b + 1) * LANES)
        normed[:, here] = (tok[:, here].astype(F32) * factor * gain32[0, b:b + 1, :]).astype(BF16)
    share = 2 * depth
    for yy in range(ny):
        if share < LANES:
            per = LANES // share
            for m in range(nz // per):
                parts = []
                for i in range(per):
                    start = ((m * per + i) * ny + yy) * share
                    block = normed[:, start // LANES * LANES:(start // LANES + 1) * LANES].astype(F32)
                    turn = (i * share - start % LANES) % LANES
                    parts.append(pltpu.roll(block, turn, 1) if turn else block)
                lane = iota((rows, LANES), 1)
                merged = parts[0]
                for i in range(1, per):
                    merged = jnp.where(lane >= i * share, parts[i], merged)
                asend[yy, :, m * LANES:(m + 1) * LANES] = merged.astype(BF16)
        else:
            for m in range(nz):
                start = (m * ny + yy) * share
                asend[yy, :, m * share:(m + 1) * share] = normed[:, start:start + share]
    a_copies = []
    for dy in range(1, ny):
        yy = lax.rem(y + dy, ny)
        a_copies.append(remote(asend.at[yy], arecv.at[y], (at(z, yy), t)))
    arecv[y] = asend[y]

    wide_n = blocks * rows
    eid = iota((chips, rows), 0)
    before = (iota((rows, rows), 0) < iota((rows, rows), 1)).astype(F32)
    hot = [(ids[k:k + 1, :] == eid).astype(F32) for k in range(2)]
    totals = jnp.sum(hot[0], axis=1, keepdims=True)
    ranks = [
        jnp.sum(hot[0] * dot(hot[0], before), axis=0, keepdims=True),
        jnp.sum(hot[1] * (dot(hot[1], before) + totals), axis=0, keepdims=True),
    ]
    scale = 1.0 / (rw[0:1, :] + rw[1:2, :])
    row = iota((chips * tile, wide_n), 0)
    lane = iota((chips * tile, wide_n), 1)
    d_of, j_of, s_of = row // tile, row // CAP % blocks, row % CAP
    e_of = (z + d_of // ny) % nz * ny + (y + d_of % ny) % ny
    same = j_of == lane // rows
    hits = []
    for k in range(2):
        ids_t = jnp.concatenate([ids[k:k + 1, :]] * blocks, axis=1)
        rank_t = jnp.concatenate([ranks[k].astype(jnp.int32)] * blocks, axis=1)
        hits.append(same & (e_of == ids_t) & (s_of == rank_t))
    table[...] = (hits[0].astype(F32) + hits[1].astype(F32)).astype(BF16)
    weighted = sum(
        jnp.where(hits[k], jnp.concatenate([rw[k:k + 1, :] * scale] * blocks, axis=1), 0.0) for k in range(2)
    )
    flipped = jnp.transpose(weighted)
    table_hi[...] = flipped.astype(BF16)
    table_lo[...] = (flipped - table_hi[...].astype(F32)).astype(BF16)

    for k in range(1, max(max(reach[0]), max(reach[1])) + 1):
        for p in range(pieces):
            if k <= reach[p][0]:
                going_right[(k, p)].wait_recv()
                if k < reach[p][0]:
                    going_right[(k + 1, p)] = hop(z + nz - k, p, right, recv_right[(k + 1, p)])
                hop(z + nz - k, p, partner, handed)
            if k <= reach[p][1]:
                going_left[(k, p)].wait_recv()
                if k < reach[p][1]:
                    going_left[(k + 1, p)] = hop(z + k, p, left, recv_left[(k + 1, p)])
                hop(z + k, p, partner, handed)

    contract = (((1,), (1,)), ((), ()))
    in_all = lax.dot_general(normed[...], win[...], contract, preferred_element_type=F32)
    forget_all = lax.dot_general(normed[...], wfg[...], contract, preferred_element_type=F32)
    square[...] = jnp.zeros_like(square)
    square[0:heads, 0:rows] = stab[...]
    stab_t = jnp.transpose(square[...])
    gates = []
    for h in range(heads):
        mine = iota(in_all.shape, 1) == t * heads + h
        in_pre = jnp.sum(jnp.where(mine, in_all, 0.0), axis=1, keepdims=True) + bias_in[t * heads + h]
        forget_pre = jnp.sum(jnp.where(mine, forget_all, 0.0), axis=1, keepdims=True) + bias_forget[t * heads + h]
        lf = jnp.minimum(forget_pre, 0.0) - jnp.log1p(jnp.exp(-jnp.abs(forget_pre)))
        old = stab_t[0:rows, h:h + 1]
        new = jnp.maximum(lf + old, in_pre)
        gates.append((new, jnp.exp(lf + old - new), jnp.exp(in_pre - new)))
    for h in range(heads):
        square[0:rows, h:h + 1] = gates[h][0]
    stab_o[...] = jnp.transpose(square[...])[0:heads, 0:rows]

    for copy in a_copies:
        copy.wait_recv()
    whole = wbuf.at[:, 1 - c]
    pltpu.make_async_remote_copy(
        src_ref=whole, dst_ref=whole, send_sem=handed, recv_sem=handed, device_id=(partner, t), device_id_type=MESH
    ).wait_recv()
    features = arecv.shape[2]
    left_side = arecv[...].reshape(ny * rows, features)
    for i in range(4):
        here = slice(i * cols, (i + 1) * cols)
        part = dot(left_side, wbuf[:, :, :, here].reshape(features, cols))
        for yy in range(ny):
            psend[yy, :, here] = part[yy * rows:(yy + 1) * rows].astype(BF16)
    p_copies = []
    for dy in sorted(range(1, ny), key=lambda d: -min(d, ny - d)):
        yy = lax.rem(y + dy, ny)
        p_copies.append(remote(psend.at[yy], precv.at[dy - 1], (at(z, yy), t)))
    total = psend[y].astype(F32)
    for copy in p_copies:
        copy.wait_recv()
    for dy in range(1, ny):
        total = total + precv[dy - 1].astype(F32)
    total = total.astype(BF16).astype(F32)

    mat_in.wait()
    key_scale = head_dim ** -0.5
    query = [total[:, h * head_dim:(h + 1) * head_dim] for h in range(heads)]
    keys = [total[:, cols + h * head_dim:cols + (h + 1) * head_dim] for h in range(heads)]
    for h in range(heads):
        square[h * rows:(h + 1) * rows, :] = query[h]
        square[(heads + h) * rows:(heads + h + 1) * rows, :] = keys[h] * key_scale
    turned = jnp.transpose(square[...])
    for h in range(heads):
        for s in range(rows):
            at_s = h * rows + s
            num[h, s:s + 1, :] = jnp.sum(turned[:, at_s:at_s + 1] * mat[s, h], axis=0, keepdims=True)
    for h in range(heads):
        new, carry, inflow = gates[h]
        kk = keys[h] * key_scale
        vals = total[:, 2 * cols + h * head_dim:2 * cols + (h + 1) * head_dim]
        gate = total[:, 3 * cols + h * head_dim:3 * cols + (h + 1) * head_dim]
        weight = inflow * jnp.sum(query[h] * kk, axis=1, keepdims=True)
        numer = carry * num[h] + weight * vals
        normal = carry * nrm[:, h, :] + inflow * kk
        nrm_o[:, h, :] = normal
        denom = jnp.maximum(jnp.abs(jnp.sum(query[h] * normal, axis=1, keepdims=True)), 1.0)
        hidden = numer / denom * (1.0 / (1.0 + jnp.exp(-gate)))
        cell[:, h * head_dim:(h + 1) * head_dim] = hidden.astype(BF16)
        carry_b[h] = jnp.broadcast_to(carry, (rows, head_dim))
        vals_b[h] = inflow * vals

    wproj_in.wait()
    by_distance = sorted(range(1, nx), key=lambda d: -min(d, nx - d))
    x_copies = []
    for dx in by_distance:
        q = lax.rem(t + dx, nx)
        part = dot(cell[...], wproj[:, pl.ds(pl.multiple_of(q * quarter, quarter), quarter)])
        asrc[dx - 1] = part.astype(BF16)
        x_copies.append(remote(asrc.at[dx - 1], adst.at[dx - 1], (ep, q)))
    mine = pl.ds(pl.multiple_of(t * quarter, quarter), quarter)
    attended = dot(cell[...], wproj[:, mine]).astype(BF16).astype(F32)

    for h in range(heads):
        for s in range(rows):
            at_s = (heads + h) * rows + s
            mat[s, h] = carry_b[h, s:s + 1, :] * mat[s, h] + turned[:, at_s:at_s + 1] * vals_b[h, s:s + 1, :]
    mat_out = load(mat, mat_o)

    for copy in x_copies:
        copy.wait_recv()
    for dx in range(1, nx):
        attended = attended + adst[dx - 1].astype(F32)
    resid_bf = (tok[:, mine].astype(F32) + attended).astype(BF16)
    resid[...] = resid_bf.astype(F32)
    stacked = jnp.concatenate([resid[:, b * LANES:(b + 1) * LANES] for b in range(blocks)], axis=0).astype(BF16)
    packed = dot(table[...], stacked).astype(BF16)
    dsrc[...] = packed
    ddst[0:tile, :] = packed[0:tile]
    d_send, d_recv, r_send, r_recv = sem(), sem(), sem(), sem()

    def tile_of(ref, d):
        return ref.at[pl.ds(pl.multiple_of(d * tile, tile), tile)]

    def send_out(i, carry):
        d = chips - i
        pltpu.make_async_remote_copy(
            src_ref=tile_of(dsrc, d), dst_ref=tile_of(ddst, d), send_sem=d_send, recv_sem=d_recv,
            device_id=(ahead(d), t), device_id_type=MESH,
        ).start()
        return carry

    lax.fori_loop(1, chips, send_out, 0)
    rest = slice(tile, chips * tile)
    d_all = pltpu.make_async_remote_copy(
        src_ref=dsrc.at[rest], dst_ref=ddst.at[rest], send_sem=d_send, recv_sem=d_recv, device_id=(partner, t), device_id_type=MESH
    )

    group = min(16, chips)
    span = group * tile
    per_block = group * CAP
    r_i, c_i = iota((span, span), 0), iota((span, span), 1)
    to_rows = (c_i == r_i % per_block // CAP * tile + r_i // per_block * CAP + r_i % CAP).astype(F32).astype(BF16)
    to_tiles = (c_i == r_i // CAP % blocks * per_block + r_i // tile * CAP + r_i % CAP).astype(F32).astype(BF16)
    for copy in experts_in:
        copy.wait()
    d_all.wait_recv()
    for g in range(chips // group):
        seen = dot(to_rows, ddst[g * span:(g + 1) * span, :]).astype(BF16)
        for b in range(blocks):
            xrows0[0, g * per_block:(g + 1) * per_block, b * LANES:(b + 1) * LANES] = seen[b * per_block:(b + 1) * per_block]

    xg_copies = {dx: remote(xrows0.at[0], xrows0.at[dx], (ep, lax.rem(t + dx, nx))) for dx in by_distance}
    across = {0: remote(xrows0.at[0], xrows1.at[0], (partner, t))}
    squares = [jnp.zeros((slots, 1), F32), jnp.zeros((slots, 1), F32)]

    def take(ref, dx, side):
        q = lax.rem(t + nx - dx, nx)
        fine = []
        for b in range(blocks):
            x = ref[dx, :, b * LANES:(b + 1) * LANES].astype(F32)
            squares[side] = squares[side] + jnp.sum(x * x, axis=1, keepdims=True)
            fine.append((x * gain32[1, pl.ds(q * blocks + b, 1), :]).astype(BF16))
        product = dot(jnp.concatenate(fine, axis=1), wgu[pl.ds(pl.multiple_of(q * quarter, quarter), quarter), :])
        if dx == 0:
            acc[side] = product
        else:
            acc[side] = acc[side] + product

    take(xrows0, 0, 0)
    across[0].wait_recv()
    take(xrows1, 0, 1)
    for dx in reversed(by_distance):
        xg_copies[dx].wait_recv()
        across[dx] = remote(xrows0.at[dx], xrows1.at[dx], (partner, t))
        take(xrows0, dx, 0)
    for dx in reversed(by_distance):
        across[dx].wait_recv()
        take(xrows1, dx, 1)
    inner = []
    for side in range(2):
        factor = lax.rsqrt(squares[side] * (1.0 / width) + norm_epsilon)
        gate, up = acc[side, :, 0:ffl] * factor, acc[side, :, ffl:2 * ffl] * factor
        inner.append((gate * (1.0 / (1.0 + jnp.exp(-gate))) * up).astype(BF16))

    order = by_distance + [0]
    down_copies = {}
    for dx in order:
        q = lax.rem(t + dx, nx)
        wcols = pl.ds(pl.multiple_of(q * quarter, quarter), quarter)
        csrc[dx] = dot(inner[1], wdown[:, wcols]).astype(BF16)
        down_copies[dx] = remote(csrc.at[dx], cdst.at[dx], (partner, t))
    s_copies = []
    for dx in order:
        q = lax.rem(t + dx, nx)
        wcols = pl.ds(pl.multiple_of(q * quarter, quarter), quarter)
        part = dot(inner[0], wdown[:, wcols])
        down_copies[dx].wait_recv()
        part = part + cdst[dx].astype(F32)
        if dx:
            ssrc[dx - 1] = part.astype(BF16)
            s_copies.append(remote(ssrc.at[dx - 1], sdst.at[dx - 1], (ep, q)))
        else:
            own_sum[...] = part
    for copy in s_copies:
        copy.wait_recv()
    back = own_sum[...]
    for dx in range(1, nx):
        back = back + sdst[dx - 1].astype(F32)
    back = back.astype(BF16)

    for g in range(chips // group):
        part = back[g * per_block:(g + 1) * per_block]
        seen = jnp.concatenate([part[:, b * LANES:(b + 1) * LANES] for b in range(blocks)], axis=0)
        rsrc[g * span:(g + 1) * span, :] = dot(to_tiles, seen).astype(BF16)
    rdst[0:tile, :] = rsrc[0:tile, :]

    def send_back(i, carry):
        d = chips - i
        pltpu.make_async_remote_copy(
            src_ref=tile_of(rsrc, d), dst_ref=tile_of(rdst, d), send_sem=r_send, recv_sem=r_recv,
            device_id=(behind(d), t), device_id_type=MESH,
        ).start()
        return carry

    lax.fori_loop(1, chips, send_back, 0)
    r_all = pltpu.make_async_remote_copy(
        src_ref=rsrc.at[rest], dst_ref=rdst.at[rest], send_sem=r_send, recv_sem=r_recv, device_id=(partner, t), device_id_type=MESH
    )
    for copy in sending:
        copy.wait_send()
    d_all.wait_send()
    mat_out.wait()
    r_all.wait_recv()
    routed = dot(table_hi[...], rdst[...]) + dot(table_lo[...], rdst[...])
    for b in range(blocks):
        here = slice(b * LANES, (b + 1) * LANES)
        mixed_o[:, here] = (resid[:, here] + routed[b * rows:(b + 1) * rows]).astype(BF16)
    r_all.wait_send()
    assert used[0] <= sems.shape[0], used


def body(
    tokens, gain_mix, gain_ffn, w_query, w_key, w_value, w_outgate, w_ingate, w_forget, bias_in, bias_forget,
    w_proj, matrix_state, normal_state, stab_state, route_ids, route_weights, w_exp_gate, w_exp_up, w_exp_down,
):
    ep_count, nx = lax.axis_size("ep"), lax.axis_size("tp")
    ny = 4 if ep_count == 64 else 2
    nz = ep_count // 2 // ny
    chips = nz * ny
    rows, width = tokens.shape
    heads, head_dim = matrix_state.shape[1:3]
    depth, cols = w_query.shape
    ffl = w_exp_gate.shape[2]
    quarter = width // nx
    blocks = quarter // LANES
    tile = blocks * CAP
    slots = chips * CAP
    share = 2 * depth * nz
    cfg = (nz, ny, nx, rows, depth, width, ffl, heads)
    hbm = pl.BlockSpec(memory_space=pl.ANY)
    smem = pl.BlockSpec(memory_space=pltpu.SMEM)
    vmem = pl.BlockSpec(memory_space=pltpu.VMEM)
    V = pltpu.VMEM
    xs = max(nx - 1, 1)
    mixed, matrix_new, normal_new, stab_new = pl.pallas_call(
        functools.partial(layer_kernel, cfg),
        out_shape=(
            jax.ShapeDtypeStruct((rows, quarter), BF16),
            jax.ShapeDtypeStruct(matrix_state.shape, F32),
            jax.ShapeDtypeStruct(normal_state.shape, F32),
            jax.ShapeDtypeStruct((heads, rows), F32),
        ),
        in_specs=[hbm] * 9 + [smem] * 2 + [hbm] * 9,
        out_specs=(vmem, hbm, vmem, vmem),
        scratch_shapes=[
            V((rows, width), BF16), V((width // LANES, LANES), BF16), V((width // LANES, LANES), BF16),
            V((nx * heads, width), BF16), V((nx * heads, width), BF16), V((cols, width), BF16),
            V(matrix_state.shape, F32), V(normal_state.shape, F32), V((heads, rows), F32),
            V((2, rows), jnp.int32), V((2, rows), F32), V((width, 2 * ffl), BF16), V((ffl, width), BF16),
            V((nz, 2, depth, 4 * cols), BF16), V((ny, rows, share), BF16), V((ny, rows, share), BF16),
            V((ny, rows, 4 * cols), BF16), V((ny - 1, rows, 4 * cols), BF16), V((rows, width), BF16),
            V((LANES, LANES), F32), V((heads, rows, head_dim), F32), V((heads, rows, head_dim), F32),
            V((heads, rows, head_dim), F32), V((rows, cols), BF16), V((2, width // LANES, LANES), F32),
            V((xs, rows, quarter), BF16), V((xs, rows, quarter), BF16), V((rows, quarter), F32),
            V((chips * tile, blocks * rows), BF16), V((blocks * rows, chips * tile), BF16), V((blocks * rows, chips * tile), BF16),
            V((chips * tile, LANES), BF16), V((chips * tile, LANES), BF16),
            V((nx, slots, quarter), BF16), V((nx, slots, quarter), BF16), V((2, slots, 2 * ffl), F32),
            V((nx, slots, quarter), BF16), V((nx, slots, quarter), BF16), V((slots, quarter), F32),
            V((xs, slots, quarter), BF16), V((xs, slots, quarter), BF16),
            V((chips * tile, LANES), BF16), V((chips * tile, LANES), BF16),
            pltpu.SemaphoreType.DMA((160,)),
        ],
        compiler_params=pltpu.CompilerParams(collective_id=0, has_side_effects=True),
    )(
        tokens, gain_mix.reshape(-1, LANES), gain_ffn.reshape(-1, LANES), w_query, w_key, w_value, w_outgate,
        w_ingate.T, w_forget.T, bias_in, bias_forget, w_proj, matrix_state, normal_state, stab_state.T,
        route_ids.T, route_weights.T, w_exp_gate, w_exp_up, w_exp_down,
    )
    return mixed, matrix_new, normal_new, stab_new.T


def solution(mesh):
    placed = (
        P("ep", None), P(), P(), P("ep", "tp"), P("ep", "tp"), P("ep", "tp"), P("ep", "tp"), P(), P(), P(), P(),
        P("tp", None), P("ep", "tp", None, None), P("ep", "tp", None), P("ep", "tp"), P("ep", None), P("ep", None),
        P("ep", None, "tp"), P("ep", None, "tp"), P("ep", "tp", None),
    )
    return jax.shard_map(
        body,
        mesh=mesh,
        in_specs=placed,
        out_specs=(P("ep", "tp"), P("ep", "tp", None, None), P("ep", "tp", None), P("ep", "tp")),
        check_vma=False,
    )
```

```python
import functools
import jax
import jax.numpy as jnp
from jax import lax
from jax.experimental import pallas as pl
from jax.experimental.pallas import tpu as pltpu
from jax.sharding import PartitionSpec as P

norm_epsilon = 1e-06
CAP = 4
PIECES = 4
FINISH = 4
LANES = 128
F32, BF16 = jnp.float32, jnp.bfloat16
MESH = pl.DeviceIdType.MESH


def iota(shape, dim):
    return lax.broadcasted_iota(jnp.int32, shape, dim)


def dot(a, b):
    return jnp.dot(a, b, preferred_element_type=F32)


def layer_kernel(
    cfg,
    tokens_h, gain_mix_h, gain_ffn_h, wq_h, wk_h, wv_h, wo_h, win_h, wfg_h, bias_in_h, bias_forget_h,
    wproj_h, mat_h, nrm_h, stab_h, ids_h, rw_h, wgate_h, wup_h, wdown_h,
    mixed_o, mat, nrm_o, stab_o,
    tok, gmix, gffn, win, wfg, bias_in, bias_forget, wproj, nrm, stab, ids, rw, wgu, wdown,
    wbuf, asend, arecv, psend, precv, normed, square, carry_b, vals_b, num, cell, gain32,
    asrc, adst, resid, table, table_hi, table_lo, dsrc, ddst, xrows0, xrows1, acc, csrc, cdst, own_sum,
    ssrc, sdst, rsrc, rdst,
    sems,
):
    nz, ny, nx, rows, depth, width, ffl, heads = cfg
    ep, t = lax.axis_index("ep"), lax.axis_index("tp")
    c = lax.rem(ep, 2)
    y = lax.rem(lax.div(ep, 2), ny)
    z = lax.div(ep, 2 * ny)
    chips = nz * ny
    quarter = width // nx
    blocks = quarter // LANES
    tile = blocks * CAP
    slots = chips * CAP
    head_dim = LANES
    cols = heads * head_dim

    def at(zz, yy):
        return (lax.rem(zz, nz) * ny + lax.rem(yy, ny)) * 2 + c

    def ahead(d):
        return at(z + lax.div(d, ny), y + lax.rem(d, ny))

    def behind(d):
        return at(z + nz - lax.div(d, ny), y + ny - lax.rem(d, ny))

    partner = ep + 1 - 2 * c
    open_scope = []

    def phase(name):
        if open_scope:
            open_scope.pop().__exit__(None, None, None)
        if name:
            open_scope.append(jax.named_scope(name))
            open_scope[0].__enter__()

    used = [0]
    sending = []

    def sem():
        used[0] += 1
        return sems.at[used[0] - 1]

    def load(src, dst):
        copy = pltpu.make_async_copy(src, dst, sem())
        copy.start()
        return copy

    def remote(src, dst, to, recv=None):
        copy = pltpu.make_async_remote_copy(
            src_ref=src, dst_ref=dst, send_sem=sem(), recv_sem=sem() if recv is None else recv,
            device_id=to, device_id_type=MESH,
        )
        copy.start()
        sending.append(copy)
        return copy

    phase("loads")
    weights = [load(w, wbuf.at[z, c, :, i * cols:(i + 1) * cols]) for i, w in enumerate((wq_h, wk_h, wv_h, wo_h))]
    early = [load(a, b) for a, b in ((tokens_h, tok), (gain_mix_h, gmix), (ids_h, ids), (rw_h, rw), (win_h, win), (wfg_h, wfg), (bias_in_h, bias_in), (bias_forget_h, bias_forget), (stab_h, stab), (nrm_h, nrm), (gain_ffn_h, gffn))]
    mat_in = load(mat_h, mat)
    wproj_in = load(wproj_h, wproj)
    experts_in = [load(wgate_h.at[0], wgu.at[:, 0:ffl]), load(wup_h.at[0], wgu.at[:, ffl:2 * ffl]), load(wdown_h.at[0], wdown)]

    phase("barrier")
    barrier = pltpu.get_barrier_semaphore()

    def greet(d, carry):
        pl.semaphore_signal(barrier, inc=1, device_id=(ahead(d), t), device_id_type=MESH)
        return carry

    lax.fori_loop(1, chips, greet, 0)
    for dx in range(1, nx):
        pl.semaphore_signal(barrier, inc=1, device_id=(ep, lax.rem(t + dx, nx)), device_id_type=MESH)
    pl.semaphore_signal(barrier, inc=1, device_id=(partner, t), device_id_type=MESH)
    pl.semaphore_wait(barrier, chips - 1 + nx - 1 + 1)

    phase("wait_w")
    for copy in weights:
        copy.wait()
    phase("ring_start")
    right, left = at(z + 1, y), at(z + nz - 1, y)
    pieces = PIECES
    pcols = 4 * cols // pieces
    reach = [(nz // 2, nz - 1 - nz // 2), (nz - 1 - nz // 2, nz // 2)] * (pieces // 2)
    handed = sem()

    def piece(zz, p):
        return wbuf.at[lax.rem(zz, nz), c, :, p * pcols:(p + 1) * pcols]

    def hop(zz, p, to, recv):
        return remote(piece(zz, p), piece(zz, p), (to, t), recv)

    going_right, going_left = {}, {}
    recv_right = {(k, p): sem() for p in range(pieces) for k in range(1, reach[p][0] + 1)}
    recv_left = {(k, p): sem() for p in range(pieces) for k in range(1, reach[p][1] + 1)}
    for p in range(pieces):
        if reach[p][0] >= 1:
            going_right[(1, p)] = hop(z, p, right, recv_right[(1, p)])
        if reach[p][1] >= 1:
            going_left[(1, p)] = hop(z, p, left, recv_left[(1, p)])
    for p in range(pieces):
        hop(z, p, partner, handed)

    phase("norm")
    for copy in early:
        copy.wait()
    wide = tok[...].astype(F32)
    factor = lax.rsqrt(jnp.sum(wide * wide, axis=-1, keepdims=True) * (1.0 / width) + norm_epsilon)
    gain32[0] = gmix[...].astype(F32)
    gain32[1] = gffn[...].astype(F32)
    for b in range(width // LANES):
        here = slice(b * LANES, (b + 1) * LANES)
        normed[:, here] = (tok[:, here].astype(F32) * factor * gain32[0, b:b + 1, :]).astype(BF16)
    share = 2 * depth
    for yy in range(ny):
        if share < LANES:
            per = LANES // share
            for m in range(nz // per):
                parts = []
                for i in range(per):
                    start = ((m * per + i) * ny + yy) * share
                    block = normed[:, start // LANES * LANES:(start // LANES + 1) * LANES].astype(F32)
                    turn = (i * share - start % LANES) % LANES
                    parts.append(pltpu.roll(block, turn, 1) if turn else block)
                lane = iota((rows, LANES), 1)
                merged = parts[0]
                for i in range(1, per):
                    merged = jnp.where(lane >= i * share, parts[i], merged)
                asend[yy, :, m * LANES:(m + 1) * LANES] = merged.astype(BF16)
        else:
            for m in range(nz):
                start = (m * ny + yy) * share
                asend[yy, :, m * share:(m + 1) * share] = normed[:, start:start + share]
    phase("a_send")
    a_copies = []
    for dy in range(1, ny):
        yy = lax.rem(y + dy, ny)
        a_copies.append(remote(asend.at[yy], arecv.at[y], (at(z, yy), t)))
    arecv[y] = asend[y]

    phase("tables")
    wide_n = blocks * rows
    eid = iota((chips, rows), 0)
    before = (iota((rows, rows), 0) < iota((rows, rows), 1)).astype(F32)
    hot = [(ids[k:k + 1, :] == eid).astype(F32) for k in range(2)]
    totals = jnp.sum(hot[0], axis=1, keepdims=True)
    ranks = [
        jnp.sum(hot[0] * dot(hot[0], before), axis=0, keepdims=True),
        jnp.sum(hot[1] * (dot(hot[1], before) + totals), axis=0, keepdims=True),
    ]
    scale = 1.0 / (rw[0:1, :] + rw[1:2, :])
    row = iota((chips * tile, wide_n), 0)
    lane = iota((chips * tile, wide_n), 1)
    d_of, j_of, s_of = row // tile, row // CAP % blocks, row % CAP
    e_of = (z + d_of // ny) % nz * ny + (y + d_of % ny) % ny
    same = j_of == lane // rows
    hits = []
    for k in range(2):
        ids_t = jnp.concatenate([ids[k:k + 1, :]] * blocks, axis=1)
        rank_t = jnp.concatenate([ranks[k].astype(jnp.int32)] * blocks, axis=1)
        hits.append(same & (e_of == ids_t) & (s_of == rank_t))
    table[...] = (hits[0].astype(F32) + hits[1].astype(F32)).astype(BF16)
    weighted = sum(
        jnp.where(hits[k], jnp.concatenate([rw[k:k + 1, :] * scale] * blocks, axis=1), 0.0) for k in range(2)
    )
    flipped = jnp.transpose(weighted)
    table_hi[...] = flipped.astype(BF16)
    table_lo[...] = (flipped - table_hi[...].astype(F32)).astype(BF16)

    phase("ring")
    for k in range(1, max(max(reach[0]), max(reach[1])) + 1):
        for p in range(pieces):
            if k <= reach[p][0]:
                going_right[(k, p)].wait_recv()
                if k < reach[p][0]:
                    going_right[(k + 1, p)] = hop(z + nz - k, p, right, recv_right[(k + 1, p)])
                hop(z + nz - k, p, partner, handed)
            if k <= reach[p][1]:
                going_left[(k, p)].wait_recv()
                if k < reach[p][1]:
                    going_left[(k + 1, p)] = hop(z + k, p, left, recv_left[(k + 1, p)])
                hop(z + k, p, partner, handed)

    phase("gates")
    contract = (((1,), (1,)), ((), ()))
    in_all = lax.dot_general(normed[...], win[...], contract, preferred_element_type=F32)
    forget_all = lax.dot_general(normed[...], wfg[...], contract, preferred_element_type=F32)
    square[...] = jnp.zeros_like(square)
    square[0:heads, 0:rows] = stab[...]
    stab_t = jnp.transpose(square[...])
    gates = []
    for h in range(heads):
        mine = iota(in_all.shape, 1) == t * heads + h
        in_pre = jnp.sum(jnp.where(mine, in_all + bias_in[...], 0.0), axis=1, keepdims=True)
        forget_pre = jnp.sum(jnp.where(mine, forget_all + bias_forget[...], 0.0), axis=1, keepdims=True)
        lf = jnp.minimum(forget_pre, 0.0) - jnp.log1p(jnp.exp(-jnp.abs(forget_pre)))
        old = stab_t[0:rows, h:h + 1]
        new = jnp.maximum(lf + old, in_pre)
        gates.append((new, jnp.exp(lf + old - new), jnp.exp(in_pre - new)))
    for h in range(heads):
        square[0:rows, h:h + 1] = gates[h][0]
    stab_o[...] = jnp.transpose(square[...])[0:heads, 0:rows]

    phase("wait_a")
    for copy in a_copies:
        copy.wait_recv()
    phase("wait_handed")
    whole = wbuf.at[:, 1 - c]
    pltpu.make_async_remote_copy(
        src_ref=whole, dst_ref=whole, send_sem=handed, recv_sem=handed, device_id=(partner, t), device_id_type=MESH
    ).wait_recv()
    phase("project")
    features = arecv.shape[2]
    left_side = arecv[...].reshape(ny * rows, features)
    p_copies = [[], []]
    for i in range(4):
        here = slice(i * cols, (i + 1) * cols)
        part = dot(left_side, wbuf[:, :, :, here].reshape(features, cols))
        for yy in range(ny):
            psend[yy, :, here] = part[yy * rows:(yy + 1) * rows].astype(BF16)
        if i in (0, 3):
            span = slice(0, cols) if i == 0 else slice(cols, 4 * cols)
            for dy in sorted(range(1, ny), key=lambda d: -min(d, ny - d)):
                yy = lax.rem(y + dy, ny)
                p_copies[i // 3].append(remote(psend.at[yy, :, span], precv.at[dy - 1, :, span], (at(z, yy), t)))

    def summed(half, span):
        total = psend[y, :, span].astype(F32)
        for copy in p_copies[half]:
            copy.wait_recv()
        for dy in range(1, ny):
            total = total + precv[dy - 1, :, span].astype(F32)
        return total.astype(BF16).astype(F32)

    phase("wait_q")
    q_all = summed(0, slice(0, cols))
    phase("numer")
    mat_in.wait()
    key_scale = head_dim ** -0.5
    query = [q_all[:, h * head_dim:(h + 1) * head_dim] for h in range(heads)]
    square[...] = jnp.zeros_like(square)
    for h in range(heads):
        square[h * rows:(h + 1) * rows, :] = query[h]
    turned = jnp.transpose(square[...])
    for h in range(heads):
        for s in range(rows):
            at_s = h * rows + s
            column = turned[:, at_s:at_s + 1]
            sums = [column[i * 8:(i + 1) * 8] * mat[s, h, i * 8:(i + 1) * 8, :] for i in range(head_dim // 8)]
            while len(sums) > 1:
                sums = [sums[i] + sums[i + 1] for i in range(0, len(sums), 2)]
            num[h, s * 8:(s + 1) * 8, :] = sums[0]
    phase("wait_kvo")
    others = summed(1, slice(cols, 4 * cols))
    keys = [others[:, h * head_dim:(h + 1) * head_dim] for h in range(heads)]
    phase("cell")
    for h in range(heads):
        new, carry, inflow = gates[h]
        kk = keys[h] * key_scale
        vals = others[:, cols + h * head_dim:cols + (h + 1) * head_dim]
        gate = others[:, 2 * cols + h * head_dim:2 * cols + (h + 1) * head_dim]
        weight = inflow * jnp.sum(query[h] * kk, axis=1, keepdims=True)
        folded = num[h, pl.ds(0, rows, stride=8), :]
        for i in range(1, 8):
            folded = folded + num[h, pl.ds(i, rows, stride=8), :]
        numer = carry * folded + weight * vals
        normal = carry * nrm[:, h, :] + inflow * kk
        nrm_o[:, h, :] = normal
        denom = jnp.maximum(jnp.abs(jnp.sum(query[h] * normal, axis=1, keepdims=True)), 1.0)
        hidden = numer / denom * (1.0 / (1.0 + jnp.exp(-gate)))
        cell[:, h * head_dim:(h + 1) * head_dim] = hidden.astype(BF16)
        carry_b[h] = jnp.broadcast_to(carry, (rows, head_dim))
        vals_b[h] = inflow * vals

    phase("outproj")
    wproj_in.wait()
    by_distance = sorted(range(1, nx), key=lambda d: -min(d, nx - d))
    x_copies = []
    for dx in by_distance:
        q = lax.rem(t + dx, nx)
        part = dot(cell[...], wproj[:, pl.ds(pl.multiple_of(q * quarter, quarter), quarter)])
        asrc[dx - 1] = part.astype(BF16)
        x_copies.append(remote(asrc.at[dx - 1], adst.at[dx - 1], (ep, q)))
    mine = pl.ds(pl.multiple_of(t * quarter, quarter), quarter)
    attended = dot(cell[...], wproj[:, mine]).astype(BF16).astype(F32)

    phase("update")
    for h in range(heads):
        square[h * rows:(h + 1) * rows, :] = keys[h] * key_scale
    turned = jnp.transpose(square[...])
    for h in range(heads):
        for s in range(rows):
            at_s = h * rows + s
            mat[s, h] = carry_b[h, s:s + 1, :] * mat[s, h] + turned[:, at_s:at_s + 1] * vals_b[h, s:s + 1, :]

    phase("wait_x")
    for copy in x_copies:
        copy.wait_recv()
    phase("dispatch")
    for dx in range(1, nx):
        attended = attended + adst[dx - 1].astype(F32)
    resid_bf = (tok[:, mine].astype(F32) + attended).astype(BF16)
    resid[...] = resid_bf.astype(F32)
    stacked = jnp.concatenate([resid[:, b * LANES:(b + 1) * LANES] for b in range(blocks)], axis=0).astype(BF16)
    packed = dot(table[...], stacked).astype(BF16)
    dsrc[...] = packed
    ddst[0:tile, :] = packed[0:tile]
    d_send, d_recv, r_send, r_recv = sem(), sem(), sem(), sem()

    def tile_of(ref, d):
        return ref.at[d * tile:(d + 1) * tile]

    far = [min(d // ny, nz - d // ny) + min(d % ny, ny - d % ny) for d in range(chips)]
    far_first = sorted(range(1, chips), key=lambda d: -far[d])

    def scatter(src, dst, send, recv, where):
        for d in far_first:
            pltpu.make_async_remote_copy(
                src_ref=tile_of(src, d), dst_ref=tile_of(dst, d), send_sem=send, recv_sem=recv,
                device_id=(where(d), t), device_id_type=MESH,
            ).start()

    scatter(dsrc, ddst, d_send, d_recv, ahead)
    rest = slice(tile, chips * tile)
    d_all = pltpu.make_async_remote_copy(
        src_ref=dsrc.at[rest], dst_ref=ddst.at[rest], send_sem=d_send, recv_sem=d_recv, device_id=(partner, t), device_id_type=MESH
    )

    phase("perms")
    group = min(16, chips)
    span = group * tile
    per_block = group * CAP
    r_i, c_i = iota((span, span), 0), iota((span, span), 1)
    to_rows = (c_i == r_i % per_block // CAP * tile + r_i // per_block * CAP + r_i % CAP).astype(F32).astype(BF16)
    to_tiles = (c_i == r_i // CAP % blocks * per_block + r_i // tile * CAP + r_i % CAP).astype(F32).astype(BF16)
    for copy in experts_in:
        copy.wait()
    phase("wait_d")
    d_all.wait_recv()
    phase("to_rows")
    for g in range(chips // group):
        seen = dot(to_rows, ddst[g * span:(g + 1) * span, :]).astype(BF16)
        for b in range(blocks):
            xrows0[0, g * per_block:(g + 1) * per_block, b * LANES:(b + 1) * LANES] = seen[b * per_block:(b + 1) * per_block]

    phase("gather")
    parts = 4
    prow = slots // parts
    to_right, to_left = (ep, lax.rem(t + 1, nx)), (ep, lax.rem(t + nx - 1, nx))
    from_x, across = {}, {}

    def prows(ref, dx, p):
        return ref.at[dx, p * prow:(p + 1) * prow]

    two_way = nx > 2
    for p in range(parts):
        from_x[(1, p)] = remote(prows(xrows0, 0, p), prows(xrows0, 1, p), to_right)
        if two_way:
            from_x[(nx - 1, p)] = remote(prows(xrows0, 0, p), prows(xrows0, nx - 1, p), to_left)
    across[0] = remote(xrows0.at[0], xrows1.at[0], (partner, t))
    squares = [jnp.zeros((slots, 1), F32), jnp.zeros((slots, 1), F32)]

    def take(ref, dx, side):
        q = lax.rem(t + nx - dx, nx)
        fine = []
        for b in range(blocks):
            x = ref[dx, :, b * LANES:(b + 1) * LANES].astype(F32)
            squares[side] = squares[side] + jnp.sum(x * x, axis=1, keepdims=True)
            fine.append((x * gain32[1, pl.ds(q * blocks + b, 1), :]).astype(BF16))
        product = dot(jnp.concatenate(fine, axis=1), wgu[pl.ds(pl.multiple_of(q * quarter, quarter), quarter), :])
        if dx == 0:
            acc[side] = product
        else:
            acc[side] = acc[side] + product

    def hand(dx):
        across[dx] = remote(xrows0.at[dx], xrows1.at[dx], (partner, t))

    take(xrows0, 0, 0)
    phase("relay")
    for p in range(parts):
        from_x[(1, p)].wait_recv()
        if two_way and p % 2 == 0:
            from_x[(2, p)] = remote(prows(xrows0, 1, p), prows(xrows0, 2, p), to_right)
        if two_way:
            from_x[(nx - 1, p)].wait_recv()
            if p % 2 == 1:
                from_x[(2, p)] = remote(prows(xrows0, nx - 1, p), prows(xrows0, 2, p), to_left)
    hand(1)
    if two_way:
        hand(nx - 1)
    across[0].wait_recv()
    phase("take_near")
    take(xrows1, 0, 1)
    take(xrows0, 1, 0)
    if two_way:
        take(xrows0, nx - 1, 0)
    across[1].wait_recv()
    take(xrows1, 1, 1)
    if two_way:
        across[nx - 1].wait_recv()
        take(xrows1, nx - 1, 1)
        phase("wait_far")
        for p in range(parts):
            from_x[(2, p)].wait_recv()
        hand(2)
        take(xrows0, 2, 0)
        phase("wait_far_c")
        across[2].wait_recv()
        take(xrows1, 2, 1)
    phase("inner")
    inner = []
    for side in range(2):
        factor = lax.rsqrt(squares[side] * (1.0 / width) + norm_epsilon)
        gate, up = acc[side, :, 0:ffl] * factor, acc[side, :, ffl:2 * ffl] * factor
        inner.append((gate * (1.0 / (1.0 + jnp.exp(-gate))) * up).astype(BF16))

    phase("down1")
    def down(side, dx):
        q = lax.rem(t + dx, nx)
        return dot(inner[side], wdown[:, pl.ds(pl.multiple_of(q * quarter, quarter), quarter)])

    order = ([2, 1, nx - 1] if two_way else [1]) + [0]
    down_copies, sums = {}, {}
    for dx in order:
        csrc[dx] = down(1, dx).astype(BF16)
        down_copies[dx] = remote(csrc.at[dx], cdst.at[dx], (partner, t))
    phase("down0")
    half = slots // 2
    upper, lower = slice(0, half), slice(half, slots)
    s_copies = {}

    def both(dx):
        part = down(0, dx)
        down_copies[dx].wait_recv()
        return part + cdst[dx].astype(F32)

    if two_way:
        ssrc[1] = both(2).astype(BF16)
        s_copies["ur"] = remote(ssrc.at[1, upper], sdst.at[1, upper], to_right)
        s_copies["ll"] = remote(ssrc.at[1, lower], sdst.at[1, lower], to_left)
        right_part = both(1)
        ssrc[0, lower] = right_part[lower].astype(BF16)
        s_copies["lr"] = remote(ssrc.at[0, lower], sdst.at[0, lower], to_right)
        left_part = both(nx - 1)
        ssrc[2, upper] = left_part[upper].astype(BF16)
        s_copies["ul"] = remote(ssrc.at[2, upper], sdst.at[2, upper], to_left)
        s_copies["ur"].wait_recv()
        ssrc[0, upper] = (right_part[upper] + sdst[1, upper].astype(F32)).astype(BF16)
        s_copies["ur2"] = remote(ssrc.at[0, upper], sdst.at[0, upper], to_right)
        s_copies["ll"].wait_recv()
        ssrc[2, lower] = (left_part[lower] + sdst[1, lower].astype(F32)).astype(BF16)
        s_copies["ll2"] = remote(ssrc.at[2, lower], sdst.at[2, lower], to_left)
        back = both(0)
        phase("wait_s")
        for name in ("lr", "ul", "ur2", "ll2"):
            s_copies[name].wait_recv()
        back = back + sdst[0].astype(F32) + sdst[2].astype(F32)
    else:
        ssrc[0] = both(1).astype(BF16)
        s_copies["r"] = remote(ssrc.at[0], sdst.at[0], to_right)
        back = both(0)
        s_copies["r"].wait_recv()
        back = back + sdst[0].astype(F32)
    phase("to_tiles")
    back = back.astype(BF16)

    for g in range(chips // group):
        part = back[g * per_block:(g + 1) * per_block]
        seen = jnp.concatenate([part[:, b * LANES:(b + 1) * LANES] for b in range(blocks)], axis=0)
        rsrc[g * span:(g + 1) * span, :] = dot(to_tiles, seen).astype(BF16)
    rdst[0:tile, :] = rsrc[0:tile, :]

    phase("send_back")
    scatter(rsrc, rdst, r_send, r_recv, behind)
    r_all = pltpu.make_async_remote_copy(
        src_ref=rsrc.at[rest], dst_ref=rdst.at[rest], send_sem=r_send, recv_sem=r_recv, device_id=(partner, t), device_id_type=MESH
    )
    phase("wait_sends")
    for copy in sending:
        copy.wait_send()
    d_all.wait_send()
    phase("wait_r")
    r_all.wait_recv()
    phase("combine")
    routed = dot(table_hi[...], rdst[...]) + dot(table_lo[...], rdst[...])
    for b in range(blocks):
        here = slice(b * LANES, (b + 1) * LANES)
        mixed_o[:, here] = (resid[:, here] + routed[b * rows:(b + 1) * rows]).astype(BF16)
    r_all.wait_send()
    phase(None)
    assert used[0] <= sems.shape[0], used


def finish_kernel(mixed, mat, nrm, stab, mixed_o, mat_o, nrm_o, stab_o, sems):
    per = mat.shape[0] // FINISH
    copies = [
        pltpu.make_async_copy(mat.at[i * per:(i + 1) * per], mat_o.at[i * per:(i + 1) * per], sems.at[3 + i])
        for i in range(FINISH)
    ]
    for i, (a, b) in enumerate(((mixed, mixed_o), (nrm, nrm_o), (stab, stab_o))):
        copies.append(pltpu.make_async_copy(a, b, sems.at[i]))
    for copy in copies:
        copy.start()
    for copy in copies:
        copy.wait()


def body(
    tokens, gain_mix, gain_ffn, w_query, w_key, w_value, w_outgate, w_ingate, w_forget, bias_in, bias_forget,
    w_proj, matrix_state, normal_state, stab_state, route_ids, route_weights, w_exp_gate, w_exp_up, w_exp_down,
):
    ep_count, nx = lax.axis_size("ep"), lax.axis_size("tp")
    ny = 4 if ep_count == 64 else 2
    nz = ep_count // 2 // ny
    chips = nz * ny
    rows, width = tokens.shape
    heads, head_dim = matrix_state.shape[1:3]
    depth, cols = w_query.shape
    ffl = w_exp_gate.shape[2]
    quarter = width // nx
    blocks = quarter // LANES
    tile = blocks * CAP
    slots = chips * CAP
    share = 2 * depth * nz
    cfg = (nz, ny, nx, rows, depth, width, ffl, heads)
    hbm = pl.BlockSpec(memory_space=pltpu.HBM)
    vmem = pl.BlockSpec(memory_space=pltpu.VMEM)
    V = pltpu.VMEM
    xs = max(nx - 1, 1)
    made = pl.pallas_call(
        functools.partial(layer_kernel, cfg),
        out_shape=(
            jax.ShapeDtypeStruct((rows, quarter), BF16),
            jax.ShapeDtypeStruct(matrix_state.shape, F32),
            jax.ShapeDtypeStruct(normal_state.shape, F32),
            jax.ShapeDtypeStruct((heads, rows), F32),
        ),
        in_specs=[hbm] * 20,
        out_specs=(vmem,) * 4,
        scratch_shapes=[
            V((rows, width), BF16), V((width // LANES, LANES), BF16), V((width // LANES, LANES), BF16),
            V((nx * heads, width), BF16), V((nx * heads, width), BF16), V((1, nx * heads), F32), V((1, nx * heads), F32), V((cols, width), BF16),
            V(normal_state.shape, F32), V((heads, rows), F32),
            V((2, rows), jnp.int32), V((2, rows), F32), V((width, 2 * ffl), BF16), V((ffl, width), BF16),
            V((nz, 2, depth, 4 * cols), BF16), V((ny, rows, share), BF16), V((ny, rows, share), BF16),
            V((ny, rows, 4 * cols), BF16), V((ny - 1, rows, 4 * cols), BF16), V((rows, width), BF16),
            V((LANES, LANES), F32), V((heads, rows, head_dim), F32), V((heads, rows, head_dim), F32),
            V((heads, rows * 8, head_dim), F32), V((rows, cols), BF16), V((2, width // LANES, LANES), F32),
            V((xs, rows, quarter), BF16), V((xs, rows, quarter), BF16), V((rows, quarter), F32),
            V((chips * tile, blocks * rows), BF16), V((blocks * rows, chips * tile), BF16), V((blocks * rows, chips * tile), BF16),
            V((chips * tile, LANES), BF16), V((chips * tile, LANES), BF16),
            V((nx, slots, quarter), BF16), V((nx, slots, quarter), BF16), V((2, slots, 2 * ffl), F32),
            V((nx, slots, quarter), BF16), V((nx, slots, quarter), BF16), V((8, LANES), F32),
            V((xs, slots, quarter), BF16), V((xs, slots, quarter), BF16),
            V((chips * tile, LANES), BF16), V((chips * tile, LANES), BF16),
            pltpu.SemaphoreType.DMA((240,)),
        ],
        compiler_params=pltpu.CompilerParams(collective_id=0, has_side_effects=True, vmem_limit_bytes=44 * 1024 * 1024),
    )(*[pltpu.with_memory_space_constraint(a, pltpu.HBM) for a in (
        tokens, gain_mix.reshape(-1, LANES), gain_ffn.reshape(-1, LANES), w_query, w_key, w_value, w_outgate,
        w_ingate.T, w_forget.T, bias_in.reshape(1, -1), bias_forget.reshape(1, -1), w_proj, matrix_state, normal_state, stab_state.T,
        route_ids.T, route_weights.T, w_exp_gate, w_exp_up, w_exp_down,
    )])
    mixed, matrix_new, normal_new, stab_new = pl.pallas_call(
        finish_kernel,
        out_shape=[jax.ShapeDtypeStruct(a.shape, a.dtype) for a in made],
        in_specs=[vmem] * 4,
        out_specs=[hbm] * 4,
        scratch_shapes=[pltpu.SemaphoreType.DMA((3 + FINISH,))],
        compiler_params=pltpu.CompilerParams(vmem_limit_bytes=8 * 1024 * 1024),
    )(*made)
    return mixed, matrix_new, normal_new, stab_new.T


def solution(mesh):
    placed = (
        P("ep", None), P(), P(), P("ep", "tp"), P("ep", "tp"), P("ep", "tp"), P("ep", "tp"), P(), P(), P(), P(),
        P("tp", None), P("ep", "tp", None, None), P("ep", "tp", None), P("ep", "tp"), P("ep", None), P("ep", None),
        P("ep", None, "tp"), P("ep", None, "tp"), P("ep", "tp", None),
    )
    return jax.shard_map(
        body,
        mesh=mesh,
        in_specs=placed,
        out_specs=(P("ep", "tp"), P("ep", "tp", None, None), P("ep", "tp", None), P("ep", "tp")),
        check_vma=False,
    )
```
